32 devices in a mesh: grp: 2 (over y), sp: 4 (over z), tp: 4 (over x, core).
Axes of the slice: x: 2, y: 2, z: 4, core: 2. Of those that a mesh axis runs over, the one named last changes fastest.
Arguments:
- latent: bfloat16 [3072, 2048], P(('grp', 'sp')), parts along dimension 0, may hold values from -6 to 6
- conditioning: bfloat16 [4096], P(('grp', 'sp')), parts along dimension 0, may hold values from -6 to 6
- context: bfloat16 [128, 2048], P(('grp', 'sp')), parts along dimension 0, may hold values from -6 to 6
- ctx_vector: bfloat16 [2048], P('sp'), may hold values from -6 to 6
- w_shift: bfloat16 [2048, 2048], P('sp', 'tp'), may hold values from -0.25 to 0.25
- w_scale: bfloat16 [2048, 2048], P('sp', 'tp'), may hold values from -0.25 to 0.25
- w_gate: bfloat16 [2048, 2048], P('sp', 'tp'), may hold values from -0.25 to 0.25
- norm_gain: bfloat16 [2048], replicated, may hold values from 0.099609375 to 1.8984375
- w_query: bfloat16 [2048, 1024], P(None, 'tp'), may hold values from -1 to 1
- w_key: bfloat16 [2048, 1024], P(None, 'tp'), may hold values from -1 to 1
- w_value: bfloat16 [2048, 1024], P(None, 'tp'), may hold values from -0.125 to 0.125
- offset_bias: float32 [16, 15, 31], P('tp'), may hold values from 1.5 to 4.5
- w_out: bfloat16 [1024, 2048], P(None, 'tp'), may hold values from -0.75 to 0.75
Outputs:
- mixed_out: bfloat16 [3072, 2048], P(('grp', 'sp'), 'tp'), parts along dimension 0
The draws below stay inside these ranges and needn't reach their ends.
There are 2 independent parts, one for each index of `grp`. The reference program is written for one: setup_inputs(seed, part) draws one part's arguments, and reference() takes and returns one part's arrays. A program takes and returns all parts, laid end to end along the dimension named above; an argument that names none is the same for every part. Nothing has to cross between parts.
All inputs are finite; a program needn't handle non-finite values.
Results may differ from the reference program's by a relative error of at most 0.011.
Values may be sent and summed in bfloat16 or wider, within the bound.
A program may use at most 64 MiB of HBM per device.

```python
import jax
import jax.numpy as jnp
from jax import lax

D = 2048
HEADS = 16
HEAD_DIM = 64
GRID_W = 64
WIN_H = 8
WIN_W = 16
ROWS_DEV = 6
TOKENS = 1536
CTX = 64
WIDTH = 1024
N_SP = 4


def weight_pair(key):
    base_key = jax.random.fold_in(key, 101)
    first_key, second_key = jax.random.split(base_key, 2)
    columns = HEADS * HEAD_DIM
    first = jax.random.normal(first_key, (D, columns), jnp.float32) * D ** (-0.5)
    second = jax.random.normal(second_key, (D, columns), jnp.float32) * D ** (-0.5)
    query_weight = first
    key_weight = second
    return (jnp.clip(query_weight, -1.0, 1.0), jnp.clip(key_weight, -1.0, 1.0))


def draw_w_query(key, part):
    return weight_pair(key)[0].astype(jnp.bfloat16)


def draw_w_key(key, part):
    return weight_pair(key)[1].astype(jnp.bfloat16)


def level_of(key, extent, cuts, smallest, top_value):
    gain, own = 1.0, jax.random.fold_in(key, 6)
    for dim, parts in cuts:
        heights = jnp.exp(jax.random.uniform(jax.random.fold_in(own, dim), (parts,), jnp.float32, smallest / len(cuts), top_value / len(cuts)))
        gain = gain * jnp.repeat(heights, extent[dim] // parts).reshape([-1 if axis == dim else 1 for axis in range(len(extent))])
    return gain


def noise(rng, extent, spread, reach, cuts=(), held_as=jnp.bfloat16):
    loudness = level_of(rng, extent, cuts, -0.22, 0.18) if cuts else 1.0
    values = jax.random.normal(rng, extent, jnp.float32) * spread * loudness
    return jnp.minimum(jnp.maximum(values, -reach), reach).astype(held_as)


def setup_inputs(seed: int = 0, part: int = 0) -> dict:
    streams_of = jax.random.split(jax.random.key(seed), 14)
    part_splits = jax.random.split(jax.random.fold_in(streams_of[13], part), 14)
    latent = noise(part_splits[0], (TOKENS, D), 1.0, 6.0, ((0, 4),))
    conditioning = noise(part_splits[1], (D,), 1.0, 6.0, ((0, 4),))
    context = noise(part_splits[2], (CTX, D), 1.0, 6.0, ((0, 4),))
    ctx_vector = noise(streams_of[3], (D,), 1.0, 6.0, ((0, 4),))
    w_shift = noise(streams_of[4], (D, D), (D // 4) ** -0.5, 0.25, ((0, 4), (1, 4)))
    w_scale = noise(streams_of[5], (D, D), (D // 4) ** -0.5, 0.25, ((0, 4), (1, 4)))
    w_gate = noise(streams_of[6], (D, D), (D // 4) ** -0.5, 0.25, ((0, 4), (1, 4)))
    norm_gain = jnp.clip(1.0 + 0.18 * jax.random.normal(streams_of[7], (D,), jnp.float32), 0.099609375, 1.8984375).astype(jnp.bfloat16)
    w_query = draw_w_query(jax.random.fold_in(streams_of[13], 71), part)
    w_key = draw_w_key(jax.random.fold_in(streams_of[13], 71), part)
    w_value = noise(streams_of[10], (D, WIDTH), D ** -0.5, 0.125, ((1, 4),))
    offset_bias = jnp.clip(1.5 + 3.0 * jax.random.uniform(streams_of[11], (HEADS, 2 * WIN_H - 1, 2 * WIN_W - 1), jnp.float32) ** level_of(streams_of[11], (HEADS, 2 * WIN_H - 1, 2 * WIN_W - 1), ((0, 4),), -0.2, 0.2), 1.5, 4.5)
    w_out = noise(streams_of[12], (WIDTH, D), (WIDTH // 16) ** -0.5, 0.75, ((1, 4),))
    return dict(latent=latent, conditioning=conditioning, context=context, ctx_vector=ctx_vector, w_shift=w_shift, w_scale=w_scale, w_gate=w_gate, norm_gain=norm_gain, w_query=w_query, w_key=w_key, w_value=w_value, offset_bias=offset_bias, w_out=w_out)


EPSILON = 1e-06

def modulated_norm(inputs, norm_gain, shift_vec, scale_vec):
    floats = inputs.astype(jnp.float32)
    inverse = lax.rsqrt(lax.optimization_barrier(jnp.mean(floats * floats, axis=-1, keepdims=True)) + EPSILON)
    return (floats * inverse * norm_gain.astype(jnp.float32) * (1.0 + scale_vec) + shift_vec).astype(jnp.bfloat16)

def project(inputs, weight):
    return jnp.dot(inputs, weight, preferred_element_type=jnp.float32).astype(jnp.bfloat16)

def reference(latent, conditioning, context, ctx_vector, w_shift, w_scale, w_gate, norm_gain, w_query, w_key, w_value, offset_bias, w_out):
    cond_act = jax.nn.silu(conditioning.astype(jnp.float32)).astype(jnp.bfloat16)
    ctx_act = jax.nn.silu(ctx_vector.astype(jnp.float32)).astype(jnp.bfloat16)
    shift_vec = jnp.dot(cond_act, w_shift, preferred_element_type=jnp.float32)
    scale_vec = jnp.dot(cond_act, w_scale, preferred_element_type=jnp.float32)
    gate_vec = jnp.dot(cond_act, w_gate, preferred_element_type=jnp.float32)
    ctx_shift = jnp.dot(ctx_act, w_shift, preferred_element_type=jnp.float32)
    ctx_scale = jnp.dot(ctx_act, w_scale, preferred_element_type=jnp.float32)
    normed = modulated_norm(latent, norm_gain, shift_vec, scale_vec)
    ctx_normed = modulated_norm(context, norm_gain, ctx_shift, ctx_scale)
    queries = project(normed, w_query)
    keys_lat = project(normed, w_key)
    values_lat = project(normed, w_value)
    ctx_keys = project(ctx_normed, w_key).astype(jnp.float32).reshape(-1, HEADS, HEAD_DIM)
    ctx_values = project(ctx_normed, w_value).astype(jnp.float32).reshape(-1, HEADS, HEAD_DIM)
    grid_rows = ROWS_DEV * N_SP
    query_grid = queries.astype(jnp.float32).reshape(grid_rows, GRID_W, HEADS, HEAD_DIM)
    key_grid = keys_lat.astype(jnp.float32).reshape(grid_rows, GRID_W, HEADS, HEAD_DIM)
    value_grid = values_lat.astype(jnp.float32).reshape(grid_rows, GRID_W, HEADS, HEAD_DIM)
    columns = jnp.arange(GRID_W, dtype=jnp.int32)
    col_index = jnp.clip(columns - WIN_W // 2, 0, GRID_W - WIN_W)[:, None] + jnp.arange(WIN_W, dtype=jnp.int32)[None, :]
    col_offset = (col_index - columns[:, None] + WIN_W - 1).astype(jnp.int32)
    scale_qk = HEAD_DIM ** (-0.5)
    bias_table = offset_bias.astype(jnp.float32)

    def one_row(grid_row):
        first_row = jnp.clip(grid_row - WIN_H // 2, 0, grid_rows - WIN_H).astype(jnp.int32)
        key_rows = lax.dynamic_slice_in_dim(key_grid, first_row, WIN_H, 0)
        value_rows = lax.dynamic_slice_in_dim(value_grid, first_row, WIN_H, 0)
        key_window = key_rows[:, col_index]
        value_window = value_rows[:, col_index]
        query_row = lax.dynamic_index_in_dim(query_grid, grid_row, 0, keepdims=False)
        row_offset = (first_row + jnp.arange(WIN_H, dtype=jnp.int32) - grid_row + WIN_H - 1).astype(jnp.int32)
        offset_terms = bias_table[:, row_offset[:, None, None], col_offset[None, :, :]]
        win_scores = jnp.einsum('chd,icjhd->hcij', query_row, key_window) * scale_qk + offset_terms.transpose(0, 2, 1, 3)
        ctx_scores = jnp.einsum('chd,lhd->hcl', query_row, ctx_keys) * scale_qk
        logits = jnp.concatenate([win_scores.reshape(HEADS, GRID_W, WIN_H * WIN_W), ctx_scores], axis=-1)
        rounded = jax.nn.softmax(logits, axis=-1).astype(jnp.bfloat16)
        weights = lax.optimization_barrier(rounded).astype(jnp.float32)
        win_weights = weights[..., :WIN_H * WIN_W].reshape(HEADS, GRID_W, WIN_H, WIN_W)
        result = jnp.einsum('hcij,icjhd->chd', win_weights, value_window)
        result = result + jnp.einsum('hcl,lhd->chd', weights[..., WIN_H * WIN_W:], ctx_values)
        return result.astype(jnp.bfloat16)
    attended = lax.map(one_row, jnp.arange(grid_rows, dtype=jnp.int32))
    attended = attended.reshape(grid_rows * GRID_W, HEADS * HEAD_DIM)
    branch = jnp.dot(attended, w_out, preferred_element_type=jnp.float32)
    return (latent.astype(jnp.float32) + gate_vec * branch).astype(jnp.bfloat16)
```

```python
import functools

import jax
import jax.numpy as jnp
from jax import lax
from jax.experimental import pallas as pl
from jax.experimental.pallas import tpu as pltpu
from jax.sharding import PartitionSpec as P

HEAD_DIM = 64
GRID_W = 64
WIN_H = 8
WIN_W = 16
EPSILON = 1e-06
F32 = jnp.float32
BF16 = jnp.bfloat16
MESH = pl.DeviceIdType.MESH
LOW = WIN_H // 2
HIGH = WIN_H - 1 - LOW
SPAN = WIN_H + 1
TABLE = 2 * WIN_H
PAIR = 2 * GRID_W


def silu(values):
    floats = values.astype(F32)
    return (floats / (1.0 + jnp.exp(-floats))).astype(BF16).astype(F32)


def kernel(
    n_sp,
    n_tp,
    cond_ref,
    ctxv_ref,
    gain_ref,
    context_ref,
    bias_ref,
    lat_hbm,
    wsh_hbm,
    wsc_hbm,
    wga_hbm,
    wq_hbm,
    wk_hbm,
    wv_hbm,
    wo_hbm,
    out_ref,
    lat,
    wmod,
    wqkv,
    wo,
    part,
    mod,
    inv_ref,
    normed,
    qbuf,
    kv,
    table,
    att,
    load_sem,
    part_send,
    part_recv,
    mod_send,
    mod_recv,
    ctx_send,
    ctx_recv,
    halo_send,
    halo_recv,
    att_send,
    att_recv,
):
    sp = lax.axis_index("sp")
    tp = lax.axis_index("tp")
    tokens, width = lat.shape
    head_width = wqkv.shape[2]
    cols = wmod.shape[2]
    ctx_own = context_ref.shape[0]
    rows_dev = tokens // GRID_W
    pairs = rows_dev // 2
    groups = head_width // 128
    n_ctx = ctx_own * n_sp
    own0 = LOW * GRID_W
    high0 = own0 + tokens
    ctx0 = high0 + HIGH * GRID_W

    barrier = pltpu.get_barrier_semaphore()
    for k in range(1, n_sp):
        pl.semaphore_signal(barrier, 1, device_id={"sp": lax.rem(sp + k, n_sp)}, device_id_type=MESH)
    for k in range(1, n_tp):
        pl.semaphore_signal(barrier, 1, device_id={"tp": lax.rem(tp + k, n_tp)}, device_id_type=MESH)

    loads = [
        pltpu.make_async_copy(src, dst, load_sem.at[i])
        for i, (src, dst) in enumerate(
            [
                (wsh_hbm, wmod.at[0]),
                (wsc_hbm, wmod.at[1]),
                (wga_hbm, wmod.at[2]),
                (lat_hbm, lat),
                (wk_hbm, wqkv.at[1]),
                (wv_hbm, wqkv.at[2]),
                (wq_hbm, wqkv.at[0]),
                (wo_hbm, wo),
            ]
        )
    ]
    for load in loads:
        load.start()

    row = lax.broadcasted_iota(jnp.int32, (16, cond_ref.shape[1]), 0)
    cond_act = jnp.broadcast_to(silu(cond_ref[...]), row.shape)
    ctx_act = jnp.broadcast_to(silu(ctxv_ref[...]), row.shape)
    total = None
    for m in range(3):
        acts = jnp.where(row == m, cond_act, 0.0)
        if m < 2:
            acts = jnp.where(row == m + 3, ctx_act, acts)
        loads[m].wait()
        term = jnp.dot(acts.astype(BF16), wmod[m], preferred_element_type=F32)
        total = term if total is None else total + term
    part[sp] = total[:8]

    pl.semaphore_wait(barrier, n_sp + n_tp - 2)

    def part_copy(slot, peer):
        return pltpu.make_async_remote_copy(
            src_ref=part.at[slot],
            dst_ref=part.at[slot],
            send_sem=part_send.at[peer],
            recv_sem=part_recv.at[slot],
            device_id={"sp": peer},
            device_id_type=MESH,
        )

    sp_peers = [lax.rem(sp + k, n_sp) for k in range(1, n_sp)]
    tp_peers = [lax.rem(tp + k, n_tp) for k in range(1, n_tp)]
    part_sends = [part_copy(sp, peer) for peer in sp_peers]
    for copy in part_sends:
        copy.start()

    loads[3].wait()
    for r in range(rows_dev):
        block = lat[r * GRID_W : (r + 1) * GRID_W, :].astype(F32)
        mean = jnp.mean(block * block, axis=-1, keepdims=True)
        inv_ref[r * GRID_W : (r + 1) * GRID_W, :] = jnp.broadcast_to(
            lax.rsqrt(mean + EPSILON), (GRID_W, 128)
        )
    block = context_ref[...].astype(F32)
    inv_ctx = lax.rsqrt(jnp.mean(block * block, axis=-1, keepdims=True) + EPSILON)

    key_col = lax.broadcasted_iota(jnp.int32, (GRID_W, PAIR), 0)
    lane = lax.broadcasted_iota(jnp.int32, (GRID_W, PAIR), 1)
    query_col = jnp.where(lane >= GRID_W, lane - GRID_W, lane)
    first_col = jnp.clip(query_col - WIN_W // 2, 0, GRID_W - WIN_W)
    inside = (key_col >= first_col) & (key_col < first_col + WIN_W)
    for g in range(groups):
        for hh in range(2):

            def expand(d, _, g=g, hh=hh):
                line = bias_ref[2 * g + hh, pl.ds(d, 1), :]
                turned = pltpu.roll(
                    jnp.broadcast_to(line, (GRID_W, PAIR)), 0, 1, stride=1, stride_axis=0
                )
                table[g, d, :, hh * PAIR : (hh + 1) * PAIR] = jnp.where(inside, turned, -jnp.inf)
                return 0

            lax.fori_loop(0, TABLE, expand, 0)

    @pl.when(sp == 0)
    def _():
        kv[0:own0, :] = jnp.zeros((own0, 2 * head_width), BF16)

    @pl.when(sp == n_sp - 1)
    def _():
        kv[high0:ctx0, :] = jnp.zeros((ctx0 - high0, 2 * head_width), BF16)

    for peer in sp_peers:
        part_copy(peer, peer).wait_recv()
    summed = part[0]
    for k in range(1, n_sp):
        summed = summed + part[k]
    mod[tp] = summed

    def mod_copy(slot, peer):
        return pltpu.make_async_remote_copy(
            src_ref=mod.at[slot],
            dst_ref=mod.at[slot],
            send_sem=mod_send.at[peer],
            recv_sem=mod_recv.at[slot],
            device_id={"tp": peer},
            device_id_type=MESH,
        )

    mod_sends = [mod_copy(tp, peer) for peer in tp_peers]
    for copy in mod_sends:
        copy.start()
    for copy in part_sends:
        copy.wait_send()
    for peer in tp_peers:
        mod_copy(peer, peer).wait_recv()

    for t in range(n_tp):
        span = slice(t * cols, (t + 1) * cols)
        gain = gain_ref[:, span].astype(F32)
        vectors = mod[t]
        factor, shift = gain * (1.0 + vectors[1:2]), vectors[0:1]
        ctx_factor, ctx_shift = gain * (1.0 + vectors[4:5]), vectors[3:4]
        for r in range(rows_dev):
            rows = slice(r * GRID_W, (r + 1) * GRID_W)
            normed[rows, span] = (
                lat[rows, span].astype(F32) * inv_ref[rows, 0:1] * factor + shift
            ).astype(BF16)
        normed[tokens:, span] = (
            context_ref[:, span].astype(F32) * inv_ctx * ctx_factor + ctx_shift
        ).astype(BF16)

    ctx_own_rows = pl.ds(pl.multiple_of(ctx0 + sp * ctx_own, ctx_own), ctx_own)
    for i in range(2):
        loads[4 + i].wait()
        product = jnp.dot(normed[...], wqkv[1 + i], preferred_element_type=F32).astype(BF16)
        lanes = slice(i * head_width, (i + 1) * head_width)
        kv[own0:high0, lanes] = product[:tokens]
        kv[ctx_own_rows, lanes] = product[tokens:]

    up = pltpu.make_async_remote_copy(
        src_ref=kv.at[pl.ds(high0 - own0, own0)],
        dst_ref=kv.at[pl.ds(0, own0)],
        send_sem=halo_send.at[0],
        recv_sem=halo_recv.at[0],
        device_id={"sp": lax.rem(sp + 1, n_sp)},
        device_id_type=MESH,
    )
    down = pltpu.make_async_remote_copy(
        src_ref=kv.at[pl.ds(own0, HIGH * GRID_W)],
        dst_ref=kv.at[pl.ds(high0, HIGH * GRID_W)],
        send_sem=halo_send.at[1],
        recv_sem=halo_recv.at[1],
        device_id={"sp": lax.rem(sp + n_sp - 1, n_sp)},
        device_id_type=MESH,
    )

    def ctx_copy(slot, peer):
        rows = pl.ds(pl.multiple_of(ctx0 + slot * ctx_own, ctx_own), ctx_own)
        return pltpu.make_async_remote_copy(
            src_ref=kv.at[rows],
            dst_ref=kv.at[rows],
            send_sem=ctx_send.at[peer],
            recv_sem=ctx_recv.at[slot],
            device_id={"sp": peer},
            device_id_type=MESH,
        )

    ctx_sends = [ctx_copy(sp, peer) for peer in sp_peers]
    for copy in ctx_sends:
        copy.start()

    @pl.when(sp < n_sp - 1)
    def _():
        up.start()

    @pl.when(sp > 0)
    def _():
        down.start()

    loads[6].wait()
    qbuf[...] = (
        jnp.dot(normed[:tokens], wqkv[0], preferred_element_type=F32) * HEAD_DIM ** (-0.5)
    ).astype(BF16)

    for copy in mod_sends:
        copy.wait_send()
    for peer in sp_peers:
        ctx_copy(peer, peer).wait_recv()

    @pl.when(sp > 0)
    def _():
        up.wait_recv()

    @pl.when(sp < n_sp - 1)
    def _():
        down.wait_recv()

    partner = tp + 1 - 2 * lax.rem(tp, 2)
    chips = n_tp // 2
    others = [lax.rem(tp + 2 * k, n_tp) for k in range(1, chips)]

    def att_copy(b, slot, peer, k):
        rows = pl.ds(b * PAIR, PAIR)
        return pltpu.make_async_remote_copy(
            src_ref=att.at[slot, rows],
            dst_ref=att.at[slot, rows],
            send_sem=att_send.at[b, k],
            recv_sem=att_recv.at[b, slot],
            device_id={"tp": peer},
            device_id_type=MESH,
        )

    lane_two = lax.broadcasted_iota(jnp.int32, (1, 2 * PAIR), 1)
    late = lax.rem(lane_two, PAIR) >= GRID_W
    lane_q = lax.broadcasted_iota(jnp.int32, (PAIR, 128), 1)
    grid_rows = rows_dev * n_sp
    row_base = sp * rows_dev

    def start_of(i):
        return jnp.clip(row_base + i - WIN_H // 2, 0, grid_rows - WIN_H) - row_base + LOW

    att_sends = []
    for b in range(pairs):
        i = 2 * b
        start = start_of(i)
        moved = start_of(i + 1) - start
        first = start - i + (WIN_H - 1 - LOW)
        mask_low = jnp.where(late & (moved == 1), -jnp.inf, 0.0)
        mask_high = jnp.where(late & (moved == 1), 0.0, -jnp.inf)
        window = pl.ds(pl.multiple_of(start * GRID_W, GRID_W), SPAN * GRID_W)
        for g in range(groups):
            lanes = slice(g * 128, (g + 1) * 128)
            vlanes = slice(head_width + g * 128, head_width + (g + 1) * 128)
            query = qbuf[b * PAIR : (b + 1) * PAIR, lanes]
            zero = jnp.zeros_like(query)
            stacked = jnp.concatenate(
                [jnp.where(lane_q < HEAD_DIM, query, zero), jnp.where(lane_q < HEAD_DIM, zero, query)],
                axis=0,
            )
            nt = (((1,), (1,)), ((), ()))
            tn = (((0,), (0,)), ((), ()))
            scores = lax.dot_general(kv[window, lanes], stacked, nt, preferred_element_type=F32)
            ctx_scores = lax.dot_general(
                kv[ctx0 : ctx0 + n_ctx, lanes], stacked, nt, preferred_element_type=F32
            )
            bias = table[g, pl.ds(first, SPAN)].reshape(SPAN * GRID_W, 2 * PAIR)
            scores = scores + bias
            head = scores[:GRID_W] + mask_low
            body = scores[GRID_W : WIN_H * GRID_W]
            tail = scores[WIN_H * GRID_W :] + mask_high
            pieces = [head, body, tail, ctx_scores]
            highest = functools.reduce(
                jnp.maximum, [jnp.max(piece, axis=0, keepdims=True) for piece in pieces]
            )
            pieces = [jnp.exp(piece - highest) for piece in pieces]
            sums = functools.reduce(
                jnp.add, [jnp.sum(piece, axis=0, keepdims=True) for piece in pieces]
            )
            weights = jnp.concatenate([piece.astype(BF16) for piece in pieces[:3]], axis=0)
            result = lax.dot_general(kv[window, vlanes], weights, tn, preferred_element_type=F32)
            result = result + lax.dot_general(
                kv[ctx0 : ctx0 + n_ctx, vlanes], pieces[3].astype(BF16), tn, preferred_element_type=F32
            )
            result = result / sums
            both = jnp.concatenate(
                [result[:HEAD_DIM, :PAIR], result[HEAD_DIM:, PAIR:]], axis=0
            )
            att[tp, b * PAIR : (b + 1) * PAIR, lanes] = both.T.astype(BF16)
        sends = [att_copy(b, tp, partner, 0)]
        sends += [att_copy(b, tp, peer, 1 + k) for k, peer in enumerate(others)]
        for copy in sends[1:] + sends[:1]:
            copy.start()
        att_sends += sends

    for b in range(pairs):
        for k, peer in enumerate(others):
            att_copy(b, peer, peer, 1 + k).wait_recv()
            forward = att_copy(b, peer, partner, chips + k)
            forward.start()
            att_sends.append(forward)

    loads[7].wait()
    gate = mod[tp][2:3]
    own_cols = pl.ds(pl.multiple_of(tp * cols, cols), cols)
    for b in range(pairs):
        rows = slice(b * PAIR, (b + 1) * PAIR)
        att_copy(b, partner, partner, 0).wait_recv()
        for k, peer in enumerate(others):
            source = peer + 1 - 2 * lax.rem(peer, 2)
            att_copy(b, source, partner, 0).wait_recv()
        branch = None
        for t in range(n_tp):
            term = jnp.dot(
                att[t, rows],
                wo[t * head_width : (t + 1) * head_width, :],
                preferred_element_type=F32,
            )
            branch = term if branch is None else branch + term
        out_ref[rows, :] = (lat[rows, own_cols].astype(F32) + gate * branch).astype(BF16)

    for copy in ctx_sends + att_sends:
        copy.wait_send()

    @pl.when(sp < n_sp - 1)
    def _():
        up.wait_send()

    @pl.when(sp > 0)
    def _():
        down.wait_send()


def local(
    n_sp,
    n_tp,
    latent,
    conditioning,
    context,
    ctx_vector,
    w_shift,
    w_scale,
    w_gate,
    norm_gain,
    w_query,
    w_key,
    w_value,
    offset_bias,
    w_out,
):
    tokens, width = latent.shape
    head_width = w_query.shape[1]
    cols = w_shift.shape[1]
    heads = head_width // HEAD_DIM
    ctx_own = context.shape[0]
    key_rows = tokens + (LOW + HIGH) * GRID_W + ctx_own * n_sp
    rows_dev = tokens // GRID_W
    pairs = rows_dev // 2
    chips = n_tp // 2

    turned = offset_bias[:, :, ::-1]
    early = jnp.pad(turned, ((0, 0), (0, 1), (0, 0)))
    later = jnp.pad(turned, ((0, 0), (1, 0), (0, 0)))
    reach = WIN_W - 1
    gap = jnp.zeros((heads, TABLE, GRID_W - 2 * reach - 1), F32)
    lines = jnp.concatenate(
        [early[..., reach:], gap, later, gap, early[..., :reach]], axis=-1
    )

    vmem = pl.BlockSpec(memory_space=pltpu.VMEM)
    anywhere = pl.BlockSpec(memory_space=pl.ANY)
    dma = pltpu.SemaphoreType.DMA
    return pl.pallas_call(
        functools.partial(kernel, n_sp, n_tp),
        out_shape=jax.ShapeDtypeStruct((tokens, cols), BF16),
        in_specs=[vmem] * 5 + [anywhere] * 8,
        out_specs=vmem,
        scratch_shapes=[
            pltpu.VMEM((tokens, width), BF16),
            pltpu.VMEM((3,) + w_shift.shape, BF16),
            pltpu.VMEM((3,) + w_query.shape, BF16),
            pltpu.VMEM(w_out.shape, BF16),
            pltpu.VMEM((n_sp, 8, cols), F32),
            pltpu.VMEM((n_tp, 8, cols), F32),
            pltpu.VMEM((tokens, 128), F32),
            pltpu.VMEM((tokens + ctx_own, width), BF16),
            pltpu.VMEM((tokens, head_width), BF16),
            pltpu.VMEM((key_rows, 2 * head_width), BF16),
            pltpu.VMEM((heads // 2, TABLE, GRID_W, 2 * PAIR), F32),
            pltpu.VMEM((n_tp, tokens, head_width), BF16),
            dma((8,)),
            dma((n_sp,)),
            dma((n_sp,)),
            dma((n_tp,)),
            dma((n_tp,)),
            dma((n_sp,)),
            dma((n_sp,)),
            dma((2,)),
            dma((2,)),
            dma((pairs, 2 * chips)),
            dma((pairs, n_tp)),
        ],
        compiler_params=pltpu.CompilerParams(
            collective_id=0, has_side_effects=True, vmem_limit_bytes=48 * 1024 * 1024
        ),
    )(
        conditioning.reshape(1, -1),
        ctx_vector.reshape(1, -1),
        norm_gain.reshape(1, -1),
        context,
        lines,
        latent,
        w_shift,
        w_scale,
        w_gate,
        w_query,
        w_key,
        w_value,
        w_out,
    )


def solution(mesh):
    return jax.shard_map(
        functools.partial(local, mesh.shape["sp"], mesh.shape["tp"]),
        mesh=mesh,
        in_specs=(
            P(("grp", "sp"), None),
            P(("grp", "sp")),
            P(("grp", "sp"), None),
            P("sp"),
            P("sp", "tp"),
            P("sp", "tp"),
            P("sp", "tp"),
            P(),
            P(None, "tp"),
            P(None, "tp"),
            P(None, "tp"),
            P("tp", None, None),
            P(None, "tp"),
        ),
        out_specs=P(("grp", "sp"), "tp"),
        check_vma=False,
    )
```

```python
import functools

import jax
import jax.numpy as jnp
from jax import lax
from jax.experimental import pallas as pl
from jax.experimental.pallas import tpu as pltpu
from jax.sharding import PartitionSpec as P

HEAD_DIM = 64
GRID_W = 64
WIN_H = 8
WIN_W = 16
EPSILON = 1e-06
F32 = jnp.float32
BF16 = jnp.bfloat16
MESH = pl.DeviceIdType.MESH
LOW = WIN_H // 2
HIGH = WIN_H - 1 - LOW
SPAN = WIN_H + 1
TABLE = 2 * WIN_H
PAIR = 2 * GRID_W


def silu(values):
    floats = values.astype(F32)
    return (floats / (1.0 + jnp.exp(-floats))).astype(BF16).astype(F32)


def kernel(
    n_sp,
    n_tp,
    cond_hbm,
    ctxv_hbm,
    gain_hbm,
    context_hbm,
    bias_hbm,
    lat_hbm,
    wsh_hbm,
    wsc_hbm,
    wga_hbm,
    wq_hbm,
    wk_hbm,
    wv_hbm,
    wo_hbm,
    out_ref,
    cond_ref,
    ctxv_ref,
    gain_ref,
    context_ref,
    bias_ref,
    lines,
    lat,
    wmod,
    wqkv,
    wo,
    part,
    mod,
    inv_ref,
    normed,
    qbuf,
    kv,
    table,
    att,
    load_sem,
    part_send,
    part_recv,
    mod_send,
    mod_recv,
    ctx_send,
    ctx_recv,
    halo_send,
    halo_recv,
    att_send,
    att_recv,
):
    sp = lax.axis_index("sp")
    tp = lax.axis_index("tp")
    tokens, width = lat.shape
    head_width = wqkv.shape[2]
    cols = wmod.shape[2]
    ctx_own = context_ref.shape[0]
    rows_dev = tokens // GRID_W
    pairs = rows_dev // 2
    groups = head_width // 128
    n_ctx = ctx_own * n_sp
    own0 = LOW * GRID_W
    high0 = own0 + tokens
    ctx0 = high0 + HIGH * GRID_W

    barrier = pltpu.get_barrier_semaphore()
    for k in range(1, n_sp):
        pl.semaphore_signal(barrier, 1, device_id={"sp": lax.rem(sp + k, n_sp)}, device_id_type=MESH)
    for k in range(1, n_tp):
        pl.semaphore_signal(barrier, 1, device_id={"tp": lax.rem(tp + k, n_tp)}, device_id_type=MESH)

    loads = [
        pltpu.make_async_copy(src, dst, load_sem.at[i])
        for i, (src, dst) in enumerate(
            [
                (wsh_hbm, wmod.at[0]),
                (wsc_hbm, wmod.at[1]),
                (wga_hbm, wmod.at[2]),
                (lat_hbm, lat),
                (wk_hbm, wqkv.at[1]),
                (wv_hbm, wqkv.at[2]),
                (wq_hbm, wqkv.at[0]),
                (wo_hbm, wo),
                (cond_hbm, cond_ref),
                (ctxv_hbm, ctxv_ref),
                (bias_hbm, bias_ref),
                (context_hbm, context_ref),
                (gain_hbm, gain_ref),
            ]
        )
    ]
    for load in loads[8:10] + loads[:3] + loads[10:] + loads[3:8]:
        load.start()
    for load in loads[8:10]:
        load.wait()

    row = lax.broadcasted_iota(jnp.int32, (16, cond_ref.shape[0]), 0)
    cond_act = jnp.broadcast_to(silu(cond_ref[...].reshape(1, -1)), row.shape)
    ctx_act = jnp.broadcast_to(silu(ctxv_ref[...].reshape(1, -1)), row.shape)
    total = None
    for m in range(3):
        acts = jnp.where(row == m, cond_act, 0.0)
        if m < 2:
            acts = jnp.where(row == m + 3, ctx_act, acts)
        loads[m].wait()
        term = jnp.dot(acts.astype(BF16), wmod[m], preferred_element_type=F32)
        total = term if total is None else total + term
    part[sp] = total[:8]

    pl.semaphore_wait(barrier, n_sp + n_tp - 2)

    def part_copy(slot, peer):
        return pltpu.make_async_remote_copy(
            src_ref=part.at[slot],
            dst_ref=part.at[slot],
            send_sem=part_send.at[peer],
            recv_sem=part_recv.at[slot],
            device_id={"sp": peer},
            device_id_type=MESH,
        )

    sp_peers = [lax.rem(sp + k, n_sp) for k in range(1, n_sp)]
    tp_peers = [lax.rem(tp + k, n_tp) for k in range(1, n_tp)]
    part_sends = [part_copy(sp, peer) for peer in sp_peers]
    for copy in part_sends:
        copy.start()

    for load in loads[10:]:
        load.wait()
    loads[3].wait()
    for r in range(rows_dev):
        block = lat[r * GRID_W : (r + 1) * GRID_W, :].astype(F32)
        mean = jnp.mean(block * block, axis=-1, keepdims=True)
        inv_ref[r * GRID_W : (r + 1) * GRID_W, :] = jnp.broadcast_to(
            lax.rsqrt(mean + EPSILON), (GRID_W, 128)
        )
    block = context_ref[...].astype(F32)
    inv_ctx = lax.rsqrt(jnp.mean(block * block, axis=-1, keepdims=True) + EPSILON)

    key_col = lax.broadcasted_iota(jnp.int32, (GRID_W, PAIR), 0)
    lane = lax.broadcasted_iota(jnp.int32, (GRID_W, PAIR), 1)
    query_col = jnp.where(lane >= GRID_W, lane - GRID_W, lane)
    first_col = jnp.clip(query_col - WIN_W // 2, 0, GRID_W - WIN_W)
    inside = (key_col >= first_col) & (key_col < first_col + WIN_W)
    offsets, reach = 2 * WIN_W - 1, WIN_W - 1
    source = lax.broadcasted_iota(jnp.int32, (offsets, PAIR), 0)
    target = lax.broadcasted_iota(jnp.int32, (offsets, PAIR), 1)
    early = (lax.rem(target + reach, PAIR) == offsets - 1 - source).astype(F32)
    later = (target - GRID_W + reach == offsets - 1 - source).astype(F32)
    lines[...] = jnp.zeros_like(lines)
    for h in range(2 * groups):
        exact = lax.Precision.HIGHEST
        block = bias_ref[:, h, :]
        lines[h, : TABLE - 1] = jnp.dot(block, early, precision=exact, preferred_element_type=F32)
        lines[h, 1:] += jnp.dot(block, later, precision=exact, preferred_element_type=F32)
    for g in range(groups):
        for hh in range(2):

            def expand(d, _, g=g, hh=hh):
                line = lines[2 * g + hh, pl.ds(d, 1), :]
                turned = pltpu.roll(
                    jnp.broadcast_to(line, (GRID_W, PAIR)), 0, 1, stride=1, stride_axis=0
                )
                table[g, d, :, hh * PAIR : (hh + 1) * PAIR] = jnp.where(inside, turned, -jnp.inf)
                return 0

            lax.fori_loop(0, TABLE, expand, 0)

    @pl.when(sp == 0)
    def _():
        kv[0:own0, :] = jnp.zeros((own0, 2 * head_width), BF16)

    @pl.when(sp == n_sp - 1)
    def _():
        kv[high0:ctx0, :] = jnp.zeros((ctx0 - high0, 2 * head_width), BF16)

    for peer in sp_peers:
        part_copy(peer, peer).wait_recv()
    summed = part[0]
    for k in range(1, n_sp):
        summed = summed + part[k]
    mod[tp] = summed

    def mod_copy(slot, peer):
        return pltpu.make_async_remote_copy(
            src_ref=mod.at[slot],
            dst_ref=mod.at[slot],
            send_sem=mod_send.at[peer],
            recv_sem=mod_recv.at[slot],
            device_id={"tp": peer},
            device_id_type=MESH,
        )

    mod_sends = [mod_copy(tp, peer) for peer in tp_peers]
    for copy in mod_sends:
        copy.start()
    for copy in part_sends:
        copy.wait_send()
    for peer in tp_peers:
        mod_copy(peer, peer).wait_recv()

    for t in range(n_tp):
        span = slice(t * cols, (t + 1) * cols)
        gain = gain_ref[span].astype(F32).reshape(1, -1)
        vectors = mod[t]
        factor, shift = gain * (1.0 + vectors[1:2]), vectors[0:1]
        ctx_factor, ctx_shift = gain * (1.0 + vectors[4:5]), vectors[3:4]
        for r in range(rows_dev):
            rows = slice(r * GRID_W, (r + 1) * GRID_W)
            normed[rows, span] = (
                lat[rows, span].astype(F32) * inv_ref[rows, 0:1] * factor + shift
            ).astype(BF16)
        normed[tokens:, span] = (
            context_ref[:, span].astype(F32) * inv_ctx * ctx_factor + ctx_shift
        ).astype(BF16)

    ctx_own_rows = pl.ds(pl.multiple_of(ctx0 + sp * ctx_own, ctx_own), ctx_own)
    for i in range(2):
        loads[4 + i].wait()
        product = jnp.dot(normed[...], wqkv[1 + i], preferred_element_type=F32).astype(BF16)
        lanes = slice(i * head_width, (i + 1) * head_width)
        kv[own0:high0, lanes] = product[:tokens]
        kv[ctx_own_rows, lanes] = product[tokens:]

    up = pltpu.make_async_remote_copy(
        src_ref=kv.at[pl.ds(high0 - own0, own0)],
        dst_ref=kv.at[pl.ds(0, own0)],
        send_sem=halo_send.at[0],
        recv_sem=halo_recv.at[0],
        device_id={"sp": lax.rem(sp + 1, n_sp)},
        device_id_type=MESH,
    )
    down = pltpu.make_async_remote_copy(
        src_ref=kv.at[pl.ds(own0, HIGH * GRID_W)],
        dst_ref=kv.at[pl.ds(high0, HIGH * GRID_W)],
        send_sem=halo_send.at[1],
        recv_sem=halo_recv.at[1],
        device_id={"sp": lax.rem(sp + n_sp - 1, n_sp)},
        device_id_type=MESH,
    )

    def ctx_copy(slot, peer):
        rows = pl.ds(pl.multiple_of(ctx0 + slot * ctx_own, ctx_own), ctx_own)
        return pltpu.make_async_remote_copy(
            src_ref=kv.at[rows],
            dst_ref=kv.at[rows],
            send_sem=ctx_send.at[peer],
            recv_sem=ctx_recv.at[slot],
            device_id={"sp": peer},
            device_id_type=MESH,
        )

    ctx_sends = [ctx_copy(sp, peer) for peer in sp_peers]
    for copy in ctx_sends:
        copy.start()

    @pl.when(sp < n_sp - 1)
    def _():
        up.start()

    @pl.when(sp > 0)
    def _():
        down.start()

    loads[6].wait()
    qbuf[...] = (
        jnp.dot(normed[:tokens], wqkv[0], preferred_element_type=F32) * HEAD_DIM ** (-0.5)
    ).astype(BF16)

    for copy in mod_sends:
        copy.wait_send()
    for peer in sp_peers:
        ctx_copy(peer, peer).wait_recv()

    @pl.when(sp > 0)
    def _():
        up.wait_recv()

    @pl.when(sp < n_sp - 1)
    def _():
        down.wait_recv()

    partner = tp + 1 - 2 * lax.rem(tp, 2)
    chips = n_tp // 2
    others = [lax.rem(tp + 2 * k, n_tp) for k in range(1, chips)]

    def att_copy(b, slot, peer, k):
        rows = pl.ds(b * PAIR, PAIR)
        return pltpu.make_async_remote_copy(
            src_ref=att.at[slot, rows],
            dst_ref=att.at[slot, rows],
            send_sem=att_send.at[b, k],
            recv_sem=att_recv.at[b, slot],
            device_id={"tp": peer},
            device_id_type=MESH,
        )

    lane_two = lax.broadcasted_iota(jnp.int32, (1, 2 * PAIR), 1)
    late = lax.rem(lane_two, PAIR) >= GRID_W
    lane_q = lax.broadcasted_iota(jnp.int32, (PAIR, 128), 1)
    grid_rows = rows_dev * n_sp
    row_base = sp * rows_dev

    def start_of(i):
        return jnp.clip(row_base + i - WIN_H // 2, 0, grid_rows - WIN_H) - row_base + LOW

    att_sends = []
    for b in range(pairs):
        i = 2 * b
        start = start_of(i)
        moved = start_of(i + 1) - start
        first = start - i + (WIN_H - 1 - LOW)
        mask_low = jnp.where(late & (moved == 1), -jnp.inf, 0.0)
        mask_high = jnp.where(late & (moved == 1), 0.0, -jnp.inf)
        window = pl.ds(pl.multiple_of(start * GRID_W, GRID_W), SPAN * GRID_W)
        for g in range(groups):
            lanes = slice(g * 128, (g + 1) * 128)
            vlanes = slice(head_width + g * 128, head_width + (g + 1) * 128)
            query = qbuf[b * PAIR : (b + 1) * PAIR, lanes]
            zero = jnp.zeros_like(query)
            stacked = jnp.concatenate(
                [jnp.where(lane_q < HEAD_DIM, query, zero), jnp.where(lane_q < HEAD_DIM, zero, query)],
                axis=0,
            )
            nt = (((1,), (1,)), ((), ()))
            tn = (((0,), (0,)), ((), ()))
            scores = lax.dot_general(kv[window, lanes], stacked, nt, preferred_element_type=F32)
            ctx_scores = lax.dot_general(
                kv[ctx0 : ctx0 + n_ctx, lanes], stacked, nt, preferred_element_type=F32
            )
            bias = table[g, pl.ds(first, SPAN)].reshape(SPAN * GRID_W, 2 * PAIR)
            scores = scores + bias
            head = scores[:GRID_W] + mask_low
            body = scores[GRID_W : WIN_H * GRID_W]
            tail = scores[WIN_H * GRID_W :] + mask_high
            pieces = [head, body, tail, ctx_scores]
            highest = functools.reduce(
                jnp.maximum, [jnp.max(piece, axis=0, keepdims=True) for piece in pieces]
            )
            pieces = [jnp.exp(piece - highest) for piece in pieces]
            sums = functools.reduce(
                jnp.add, [jnp.sum(piece, axis=0, keepdims=True) for piece in pieces]
            )
            weights = jnp.concatenate([piece.astype(BF16) for piece in pieces[:3]], axis=0)
            result = lax.dot_general(kv[window, vlanes], weights, tn, preferred_element_type=F32)
            result = result + lax.dot_general(
                kv[ctx0 : ctx0 + n_ctx, vlanes], pieces[3].astype(BF16), tn, preferred_element_type=F32
            )
            result = result / sums
            both = jnp.concatenate(
                [result[:HEAD_DIM, :PAIR], result[HEAD_DIM:, PAIR:]], axis=0
            )
            att[tp, b * PAIR : (b + 1) * PAIR, lanes] = both.T.astype(BF16)
        sends = [att_copy(b, tp, partner, 0)]
        sends += [att_copy(b, tp, peer, 1 + k) for k, peer in enumerate(others)]
        for copy in sends[1:] + sends[:1]:
            copy.start()
        att_sends += sends

    for b in range(pairs):
        for k, peer in enumerate(others):
            att_copy(b, peer, peer, 1 + k).wait_recv()
            forward = att_copy(b, peer, partner, chips + k)
            forward.start()
            att_sends.append(forward)

    loads[7].wait()
    gate = mod[tp][2:3]
    own_cols = pl.ds(pl.multiple_of(tp * cols, cols), cols)
    for b in range(pairs):
        rows = slice(b * PAIR, (b + 1) * PAIR)
        att_copy(b, partner, partner, 0).wait_recv()
        for k, peer in enumerate(others):
            source = peer + 1 - 2 * lax.rem(peer, 2)
            att_copy(b, source, partner, 0).wait_recv()
        branch = None
        for t in range(n_tp):
            term = jnp.dot(
                att[t, rows],
                wo[t * head_width : (t + 1) * head_width, :],
                preferred_element_type=F32,
            )
            branch = term if branch is None else branch + term
        out_ref[rows, :] = (lat[rows, own_cols].astype(F32) + gate * branch).astype(BF16)

    for copy in ctx_sends + att_sends:
        copy.wait_send()

    @pl.when(sp < n_sp - 1)
    def _():
        up.wait_send()

    @pl.when(sp > 0)
    def _():
        down.wait_send()


def local(
    n_sp,
    n_tp,
    latent,
    conditioning,
    context,
    ctx_vector,
    w_shift,
    w_scale,
    w_gate,
    norm_gain,
    w_query,
    w_key,
    w_value,
    offset_bias,
    w_out,
):
    tokens, width = latent.shape
    head_width = w_query.shape[1]
    cols = w_shift.shape[1]
    heads = head_width // HEAD_DIM
    ctx_own = context.shape[0]
    key_rows = tokens + (LOW + HIGH) * GRID_W + ctx_own * n_sp
    rows_dev = tokens // GRID_W
    pairs = rows_dev // 2
    chips = n_tp // 2

    vmem = pl.BlockSpec(memory_space=pltpu.VMEM)
    anywhere = pl.BlockSpec(memory_space=pltpu.HBM)
    dma = pltpu.SemaphoreType.DMA
    return pl.pallas_call(
        functools.partial(kernel, n_sp, n_tp),
        out_shape=jax.ShapeDtypeStruct((tokens, cols), BF16),
        in_specs=[anywhere] * 13,
        out_specs=vmem,
        scratch_shapes=[
            pltpu.VMEM(conditioning.shape, BF16),
            pltpu.VMEM(ctx_vector.shape, BF16),
            pltpu.VMEM(norm_gain.shape, BF16),
            pltpu.VMEM(context.shape, BF16),
            pltpu.VMEM((TABLE - 1, heads, 2 * WIN_W - 1), F32),
            pltpu.VMEM((heads, TABLE, PAIR), F32),
            pltpu.VMEM((tokens, width), BF16),
            pltpu.VMEM((3,) + w_shift.shape, BF16),
            pltpu.VMEM((3,) + w_query.shape, BF16),
            pltpu.VMEM(w_out.shape, BF16),
            pltpu.VMEM((n_sp, 8, cols), F32),
            pltpu.VMEM((n_tp, 8, cols), F32),
            pltpu.VMEM((tokens, 128), F32),
            pltpu.VMEM((tokens + ctx_own, width), BF16),
            pltpu.VMEM((tokens, head_width), BF16),
            pltpu.VMEM((key_rows, 2 * head_width), BF16),
            pltpu.VMEM((heads // 2, TABLE, GRID_W, 2 * PAIR), F32),
            pltpu.VMEM((n_tp, tokens, head_width), BF16),
            dma((13,)),
            dma((n_sp,)),
            dma((n_sp,)),
            dma((n_tp,)),
            dma((n_tp,)),
            dma((n_sp,)),
            dma((n_sp,)),
            dma((2,)),
            dma((2,)),
            dma((pairs, 2 * chips)),
            dma((pairs, n_tp)),
        ],
        compiler_params=pltpu.CompilerParams(
            collective_id=0, has_side_effects=True, vmem_limit_bytes=67_043_328
        ),
    )(
        conditioning,
        ctx_vector,
        norm_gain,
        context,
        offset_bias.transpose(1, 0, 2),
        latent,
        w_shift,
        w_scale,
        w_gate,
        w_query,
        w_key,
        w_value,
        w_out,
    )


def solution(mesh):
    return jax.shard_map(
        functools.partial(local, mesh.shape["sp"], mesh.shape["tp"]),
        mesh=mesh,
        in_specs=(
            P(("grp", "sp"), None),
            P(("grp", "sp")),
            P(("grp", "sp"), None),
            P("sp"),
            P("sp", "tp"),
            P("sp", "tp"),
            P("sp", "tp"),
            P(),
            P(None, "tp"),
            P(None, "tp"),
            P(None, "tp"),
            P("tp", None, None),
            P(None, "tp"),
        ),
        out_specs=P(("grp", "sp"), "tp"),
        check_vma=False,
    )
```

```python
import functools

import jax
import jax.numpy as jnp
from jax import lax
from jax.experimental import pallas as pl
from jax.experimental.pallas import tpu as pltpu
from jax.sharding import PartitionSpec as P

HEAD_DIM = 64
GRID_W = 64
WIN_H = 8
WIN_W = 16
EPSILON = 1e-06
F32 = jnp.float32
BF16 = jnp.bfloat16
MESH = pl.DeviceIdType.MESH
LOW = WIN_H // 2
HIGH = WIN_H - 1 - LOW
SPAN = WIN_H + 1
TABLE = 2 * WIN_H
PAIR = 2 * GRID_W


def silu(values):
    floats = values.astype(F32)
    return (floats / (1.0 + jnp.exp(-floats))).astype(BF16).astype(F32)


def kernel(
    n_sp,
    n_tp,
    cond_hbm,
    ctxv_hbm,
    gain_hbm,
    context_hbm,
    bias_hbm,
    lat_hbm,
    wsh_hbm,
    wsc_hbm,
    wga_hbm,
    wq_hbm,
    wk_hbm,
    wv_hbm,
    wo_hbm,
    out_ref,
    cond_ref,
    ctxv_ref,
    gain_ref,
    context_ref,
    bias_ref,
    lines,
    lat,
    wmod,
    wqkv,
    wo,
    part,
    mod,
    inv_ref,
    normed,
    qbuf,
    kv,
    table,
    att,
    load_sem,
    part_send,
    part_recv,
    mod_send,
    mod_recv,
    ctx_send,
    ctx_recv,
    halo_send,
    halo_recv,
    att_send,
    att_recv,
):
    sp = lax.axis_index("sp")
    tp = lax.axis_index("tp")
    tokens, width = lat.shape
    head_width = wqkv.shape[2]
    cols = wmod.shape[2]
    ctx_own = context_ref.shape[0]
    rows_dev = tokens // GRID_W
    pairs = rows_dev // 2
    groups = head_width // 128
    n_ctx = ctx_own * n_sp
    own0 = LOW * GRID_W
    high0 = own0 + tokens
    ctx0 = high0 + HIGH * GRID_W

    barrier = pltpu.get_barrier_semaphore()
    for k in range(1, n_sp):
        pl.semaphore_signal(barrier, 1, device_id={"sp": lax.rem(sp + k, n_sp)}, device_id_type=MESH)
    for k in range(1, n_tp):
        pl.semaphore_signal(barrier, 1, device_id={"tp": lax.rem(tp + k, n_tp)}, device_id_type=MESH)

    loads = [
        pltpu.make_async_copy(src, dst, load_sem.at[i])
        for i, (src, dst) in enumerate(
            [
                (wsh_hbm, wmod.at[0]),
                (wsc_hbm, wmod.at[1]),
                (wga_hbm, wmod.at[2]),
                (lat_hbm, lat),
                (wk_hbm, wqkv.at[1]),
                (wv_hbm, wqkv.at[2]),
                (wq_hbm, wqkv.at[0]),
                (wo_hbm, wo),
                (cond_hbm, cond_ref),
                (ctxv_hbm, ctxv_ref),
                (bias_hbm, bias_ref),
                (context_hbm, context_ref),
                (gain_hbm, gain_ref),
            ]
        )
    ]
    for load in loads[8:10] + loads[:3] + loads[10:] + loads[3:8]:
        load.start()
    for load in loads[8:10]:
        load.wait()

    row = lax.broadcasted_iota(jnp.int32, (16, cond_ref.shape[0]), 0)
    cond_act = jnp.broadcast_to(silu(cond_ref[...].reshape(1, -1)), row.shape)
    ctx_act = jnp.broadcast_to(silu(ctxv_ref[...].reshape(1, -1)), row.shape)
    total = None
    for m in range(3):
        acts = jnp.where(row == m, cond_act, 0.0)
        if m < 2:
            acts = jnp.where(row == m + 3, ctx_act, acts)
        loads[m].wait()
        term = jnp.dot(acts.astype(BF16), wmod[m], preferred_element_type=F32)
        total = term if total is None else total + term
    part[sp] = total[:8]

    pl.semaphore_wait(barrier, n_sp + n_tp - 2)

    def part_copy(slot, peer):
        return pltpu.make_async_remote_copy(
            src_ref=part.at[slot],
            dst_ref=part.at[slot],
            send_sem=part_send.at[peer],
            recv_sem=part_recv.at[slot],
            device_id={"sp": peer},
            device_id_type=MESH,
        )

    sp_peers = [lax.rem(sp + k, n_sp) for k in range(1, n_sp)]
    tp_peers = [lax.rem(tp + k, n_tp) for k in range(1, n_tp)]
    part_sends = [part_copy(sp, peer) for peer in sp_peers]
    for copy in part_sends:
        copy.start()

    for load in loads[10:]:
        load.wait()
    loads[3].wait()
    for r in range(rows_dev):
        block = lat[r * GRID_W : (r + 1) * GRID_W, :].astype(F32)
        mean = jnp.mean(block * block, axis=-1, keepdims=True)
        inv_ref[r * GRID_W : (r + 1) * GRID_W, :] = jnp.broadcast_to(
            lax.rsqrt(mean + EPSILON), (GRID_W, 128)
        )
    block = context_ref[...].astype(F32)
    inv_ctx = lax.rsqrt(jnp.mean(block * block, axis=-1, keepdims=True) + EPSILON)

    @pl.when(sp == 0)
    def _():
        kv[0:own0, :] = jnp.zeros((own0, 2 * head_width), BF16)

    @pl.when(sp == n_sp - 1)
    def _():
        kv[high0:ctx0, :] = jnp.zeros((ctx0 - high0, 2 * head_width), BF16)

    for peer in sp_peers:
        part_copy(peer, peer).wait_recv()
    summed = part[0]
    for k in range(1, n_sp):
        summed = summed + part[k]
    mod[tp] = summed

    def mod_copy(slot, peer):
        return pltpu.make_async_remote_copy(
            src_ref=mod.at[slot],
            dst_ref=mod.at[slot],
            send_sem=mod_send.at[peer],
            recv_sem=mod_recv.at[slot],
            device_id={"tp": peer},
            device_id_type=MESH,
        )

    mod_sends = [mod_copy(tp, peer) for peer in tp_peers]
    for copy in mod_sends:
        copy.start()
    for copy in part_sends:
        copy.wait_send()
    for peer in tp_peers:
        mod_copy(peer, peer).wait_recv()

    for t in range(n_tp):
        span = slice(t * cols, (t + 1) * cols)
        gain = gain_ref[span].astype(F32).reshape(1, -1)
        vectors = mod[t]
        factor, shift = gain * (1.0 + vectors[1:2]), vectors[0:1]
        ctx_factor, ctx_shift = gain * (1.0 + vectors[4:5]), vectors[3:4]
        for r in range(rows_dev):
            rows = slice(r * GRID_W, (r + 1) * GRID_W)
            normed[rows, span] = (
                lat[rows, span].astype(F32) * inv_ref[rows, 0:1] * factor + shift
            ).astype(BF16)
        normed[tokens:, span] = (
            context_ref[:, span].astype(F32) * inv_ctx * ctx_factor + ctx_shift
        ).astype(BF16)

    def halo_up(i):
        lanes = pl.ds(i * head_width, head_width)
        return pltpu.make_async_remote_copy(
            src_ref=kv.at[pl.ds(high0 - own0, own0), lanes],
            dst_ref=kv.at[pl.ds(0, own0), lanes],
            send_sem=halo_send.at[i],
            recv_sem=halo_recv.at[i],
            device_id={"sp": lax.rem(sp + 1, n_sp)},
            device_id_type=MESH,
        )

    def halo_down(i):
        lanes = pl.ds(i * head_width, head_width)
        return pltpu.make_async_remote_copy(
            src_ref=kv.at[pl.ds(own0, HIGH * GRID_W), lanes],
            dst_ref=kv.at[pl.ds(high0, HIGH * GRID_W), lanes],
            send_sem=halo_send.at[2 + i],
            recv_sem=halo_recv.at[2 + i],
            device_id={"sp": lax.rem(sp + n_sp - 1, n_sp)},
            device_id_type=MESH,
        )

    ups, downs = [halo_up(0), halo_up(1)], [halo_down(0), halo_down(1)]
    ctx_own_rows = pl.ds(pl.multiple_of(ctx0 + sp * ctx_own, ctx_own), ctx_own)
    for i in range(2):
        loads[4 + i].wait()
        product = jnp.dot(normed[...], wqkv[1 + i], preferred_element_type=F32).astype(BF16)
        lanes = slice(i * head_width, (i + 1) * head_width)
        kv[own0:high0, lanes] = product[:tokens]
        kv[ctx_own_rows, lanes] = product[tokens:]

        @pl.when(sp < n_sp - 1)
        def _(i=i):
            ups[i].start()

        @pl.when(sp > 0)
        def _(i=i):
            downs[i].start()

    def ctx_copy(slot, peer):
        rows = pl.ds(pl.multiple_of(ctx0 + slot * ctx_own, ctx_own), ctx_own)
        return pltpu.make_async_remote_copy(
            src_ref=kv.at[rows],
            dst_ref=kv.at[rows],
            send_sem=ctx_send.at[peer],
            recv_sem=ctx_recv.at[slot],
            device_id={"sp": peer},
            device_id_type=MESH,
        )

    ctx_sends = [ctx_copy(sp, peer) for peer in sp_peers]
    for copy in ctx_sends:
        copy.start()

    loads[6].wait()
    qbuf[...] = (
        jnp.dot(normed[:tokens], wqkv[0], preferred_element_type=F32) * HEAD_DIM ** (-0.5)
    ).astype(BF16)

    key_col = lax.broadcasted_iota(jnp.int32, (GRID_W, PAIR), 0)
    lane = lax.broadcasted_iota(jnp.int32, (GRID_W, PAIR), 1)
    query_col = jnp.where(lane >= GRID_W, lane - GRID_W, lane)
    first_col = jnp.clip(query_col - WIN_W // 2, 0, GRID_W - WIN_W)
    inside = (key_col >= first_col) & (key_col < first_col + WIN_W)
    offsets, reach = 2 * WIN_W - 1, WIN_W - 1
    source = lax.broadcasted_iota(jnp.int32, (offsets, PAIR), 0)
    target = lax.broadcasted_iota(jnp.int32, (offsets, PAIR), 1)
    early = (lax.rem(target + reach, PAIR) == offsets - 1 - source).astype(F32)
    later = (target - GRID_W + reach == offsets - 1 - source).astype(F32)
    lines[...] = jnp.zeros_like(lines)
    for h in range(2 * groups):
        exact = lax.Precision.HIGHEST
        block = bias_ref[:, h, :]
        lines[h, : TABLE - 1] = jnp.dot(block, early, precision=exact, preferred_element_type=F32)
        lines[h, 1:] += jnp.dot(block, later, precision=exact, preferred_element_type=F32)
    for g in range(groups):
        for hh in range(2):

            def expand(d, _, g=g, hh=hh):
                line = lines[2 * g + hh, pl.ds(d, 1), :]
                turned = pltpu.roll(
                    jnp.broadcast_to(line, (GRID_W, PAIR)), 0, 1, stride=1, stride_axis=0
                )
                table[g, d, :, hh * PAIR : (hh + 1) * PAIR] = jnp.where(inside, turned, -jnp.inf)
                return 0

            lax.fori_loop(0, TABLE, expand, 0)

    for copy in mod_sends:
        copy.wait_send()
    for peer in sp_peers:
        ctx_copy(peer, peer).wait_recv()

    @pl.when(sp < n_sp - 1)
    def _():
        for copy in downs:
            copy.wait_recv()

    @pl.when((sp > 0) & (sp == n_sp - 1))
    def _():
        for copy in ups:
            copy.wait_recv()

    partner = tp + 1 - 2 * lax.rem(tp, 2)
    chips = n_tp // 2
    others = [lax.rem(tp + 2 * k, n_tp) for k in range(1, chips)]

    def att_copy(b, slot, peer, k):
        rows = pl.ds(b * PAIR, PAIR)
        return pltpu.make_async_remote_copy(
            src_ref=att.at[slot, rows],
            dst_ref=att.at[slot, rows],
            send_sem=att_send.at[b, k],
            recv_sem=att_recv.at[b, slot],
            device_id={"tp": peer},
            device_id_type=MESH,
        )

    lane_two = lax.broadcasted_iota(jnp.int32, (1, 2 * PAIR), 1)
    late = lax.rem(lane_two, PAIR) >= GRID_W
    lane_q = lax.broadcasted_iota(jnp.int32, (PAIR, 128), 1)
    grid_rows = rows_dev * n_sp
    row_base = sp * rows_dev

    def start_of(i):
        return jnp.clip(row_base + i - WIN_H // 2, 0, grid_rows - WIN_H) - row_base + LOW

    att_sends = []
    order = list(range(pairs))[::-1]
    for turn, b in enumerate(order):
        if turn == 1:

            @pl.when((sp > 0) & (sp < n_sp - 1))
            def _():
                for copy in ups:
                    copy.wait_recv()

        i = 2 * b
        start = start_of(i)
        moved = start_of(i + 1) - start
        first = start - i + (WIN_H - 1 - LOW)
        mask_low = jnp.where(late & (moved == 1), -jnp.inf, 0.0)
        mask_high = jnp.where(late & (moved == 1), 0.0, -jnp.inf)
        window = pl.ds(pl.multiple_of(start * GRID_W, GRID_W), SPAN * GRID_W)
        for g in range(groups):
            lanes = slice(g * 128, (g + 1) * 128)
            vlanes = slice(head_width + g * 128, head_width + (g + 1) * 128)
            query = qbuf[b * PAIR : (b + 1) * PAIR, lanes]
            zero = jnp.zeros_like(query)
            stacked = jnp.concatenate(
                [jnp.where(lane_q < HEAD_DIM, query, zero), jnp.where(lane_q < HEAD_DIM, zero, query)],
                axis=0,
            )
            nt = (((1,), (1,)), ((), ()))
            tn = (((0,), (0,)), ((), ()))
            scores = lax.dot_general(kv[window, lanes], stacked, nt, preferred_element_type=F32)
            ctx_scores = lax.dot_general(
                kv[ctx0 : ctx0 + n_ctx, lanes], stacked, nt, preferred_element_type=F32
            )
            bias = table[g, pl.ds(first, SPAN)].reshape(SPAN * GRID_W, 2 * PAIR)
            scores = scores + bias
            head = scores[:GRID_W] + mask_low
            body = scores[GRID_W : WIN_H * GRID_W]
            tail = scores[WIN_H * GRID_W :] + mask_high
            pieces = [head, body, tail, ctx_scores]
            highest = functools.reduce(
                jnp.maximum, [jnp.max(piece, axis=0, keepdims=True) for piece in pieces]
            )
            pieces = [jnp.exp(piece - highest) for piece in pieces]
            sums = functools.reduce(
                jnp.add, [jnp.sum(piece, axis=0, keepdims=True) for piece in pieces]
            )
            weights = jnp.concatenate([piece.astype(BF16) for piece in pieces[:3]], axis=0)
            result = lax.dot_general(kv[window, vlanes], weights, tn, preferred_element_type=F32)
            result = result + lax.dot_general(
                kv[ctx0 : ctx0 + n_ctx, vlanes], pieces[3].astype(BF16), tn, preferred_element_type=F32
            )
            result = result / sums
            both = jnp.concatenate(
                [result[:HEAD_DIM, :PAIR], result[HEAD_DIM:, PAIR:]], axis=0
            )
            att[tp, b * PAIR : (b + 1) * PAIR, lanes] = both.T.astype(BF16)
        sends = [att_copy(b, tp, partner, 0)]
        sends += [att_copy(b, tp, peer, 1 + k) for k, peer in enumerate(others)]
        for copy in sends[1:] + sends[:1]:
            copy.start()
        att_sends += sends

    loads[7].wait()
    gate = mod[tp][2:3]
    own_cols = pl.ds(pl.multiple_of(tp * cols, cols), cols)

    def forward(b):
        for k, peer in enumerate(others):
            att_copy(b, peer, peer, 1 + k).wait_recv()
            copy = att_copy(b, peer, partner, chips + k)
            copy.start()
            att_sends.append(copy)

    forward(order[0])
    for turn, b in enumerate(order):
        if turn + 1 < pairs:
            forward(order[turn + 1])
        rows = slice(b * PAIR, (b + 1) * PAIR)
        att_copy(b, partner, partner, 0).wait_recv()
        for k, peer in enumerate(others):
            source = peer + 1 - 2 * lax.rem(peer, 2)
            att_copy(b, source, partner, 0).wait_recv()
        branch = None
        for t in range(n_tp):
            term = jnp.dot(
                att[t, rows],
                wo[t * head_width : (t + 1) * head_width, :],
                preferred_element_type=F32,
            )
            branch = term if branch is None else branch + term
        out_ref[rows, :] = (lat[rows, own_cols].astype(F32) + gate * branch).astype(BF16)

    for copy in ctx_sends + att_sends:
        copy.wait_send()

    @pl.when(sp < n_sp - 1)
    def _():
        for copy in ups:
            copy.wait_send()

    @pl.when(sp > 0)
    def _():
        for copy in downs:
            copy.wait_send()


def local(
    n_sp,
    n_tp,
    latent,
    conditioning,
    context,
    ctx_vector,
    w_shift,
    w_scale,
    w_gate,
    norm_gain,
    w_query,
    w_key,
    w_value,
    offset_bias,
    w_out,
):
    tokens, width = latent.shape
    head_width = w_query.shape[1]
    cols = w_shift.shape[1]
    heads = head_width // HEAD_DIM
    ctx_own = context.shape[0]
    key_rows = tokens + (LOW + HIGH) * GRID_W + ctx_own * n_sp
    rows_dev = tokens // GRID_W
    pairs = rows_dev // 2
    chips = n_tp // 2

    vmem = pl.BlockSpec(memory_space=pltpu.VMEM)
    anywhere = pl.BlockSpec(memory_space=pltpu.HBM)
    dma = pltpu.SemaphoreType.DMA
    return pl.pallas_call(
        functools.partial(kernel, n_sp, n_tp),
        out_shape=jax.ShapeDtypeStruct((tokens, cols), BF16),
        in_specs=[anywhere] * 13,
        out_specs=vmem,
        scratch_shapes=[
            pltpu.VMEM(conditioning.shape, BF16),
            pltpu.VMEM(ctx_vector.shape, BF16),
            pltpu.VMEM(norm_gain.shape, BF16),
            pltpu.VMEM(context.shape, BF16),
            pltpu.VMEM((TABLE - 1, heads, 2 * WIN_W - 1), F32),
            pltpu.VMEM((heads, TABLE, PAIR), F32),
            pltpu.VMEM((tokens, width), BF16),
            pltpu.VMEM((3,) + w_shift.shape, BF16),
            pltpu.VMEM((3,) + w_query.shape, BF16),
            pltpu.VMEM(w_out.shape, BF16),
            pltpu.VMEM((n_sp, 8, cols), F32),
            pltpu.VMEM((n_tp, 8, cols), F32),
            pltpu.VMEM((tokens, 128), F32),
            pltpu.VMEM((tokens + ctx_own, width), BF16),
            pltpu.VMEM((tokens, head_width), BF16),
            pltpu.VMEM((key_rows, 2 * head_width), BF16),
            pltpu.VMEM((heads // 2, TABLE, GRID_W, 2 * PAIR), F32),
            pltpu.VMEM((n_tp, tokens, head_width), BF16),
            dma((13,)),
            dma((n_sp,)),
            dma((n_sp,)),
            dma((n_tp,)),
            dma((n_tp,)),
            dma((n_sp,)),
            dma((n_sp,)),
            dma((4,)),
            dma((4,)),
            dma((pairs, 2 * chips)),
            dma((pairs, n_tp)),
        ],
        compiler_params=pltpu.CompilerParams(
            collective_id=0, has_side_effects=True, vmem_limit_bytes=67_043_328
        ),
    )(
        conditioning,
        ctx_vector,
        norm_gain,
        context,
        offset_bias.transpose(1, 0, 2),
        latent,
        w_shift,
        w_scale,
        w_gate,
        w_query,
        w_key,
        w_value,
        w_out,
    )


def solution(mesh):
    return jax.shard_map(
        functools.partial(local, mesh.shape["sp"], mesh.shape["tp"]),
        mesh=mesh,
        in_specs=(
            P(("grp", "sp"), None),
            P(("grp", "sp")),
            P(("grp", "sp"), None),
            P("sp"),
            P("sp", "tp"),
            P("sp", "tp"),
            P("sp", "tp"),
            P(),
            P(None, "tp"),
            P(None, "tp"),
            P(None, "tp"),
            P("tp", None, None),
            P(None, "tp"),
        ),
        out_specs=P(("grp", "sp"), "tp"),
        check_vma=False,
    )
```
